32 devices in a mesh: sp: 16 (over z, y, x), tp: 2 (over core).
Axes of the slice: x: 2, y: 2, z: 4, core: 2. Of those that a mesh axis runs over, the one named last changes fastest.
Arguments:
- prompt: bfloat16 [1, 8192, 2048], P(None, 'sp', 'tp'), may hold values from -6 to 6
- new_token: bfloat16 [1, 2048], P(None, 'tp'), may hold values from -6 to 6
- w_query: bfloat16 [2048, 2048], P(None, 'tp'), may hold values from -0.125 to 0.125
- w_key: bfloat16 [2048, 2048], P(None, 'tp'), may hold values from -0.125 to 0.125
- w_value: bfloat16 [2048, 2048], P(None, 'tp'), may hold values from -0.125 to 0.125
- decay_rate: float32 [16], P('tp'), may hold values from 1e-05 to 0.06
- norm_gain: float32 [2048], P('tp'), may hold values from 0.1 to 1.9
Outputs:
- mixed: bfloat16 [1, 8192, 2048], P(None, 'sp', 'tp')
- cache: bfloat16 [1, 16, 128, 128], P(None, 'tp', 'sp')
- new_read: bfloat16 [1, 2048], P(None, 'tp')
The draws below stay inside these ranges and needn't reach their ends.
All inputs are finite; a program needn't handle non-finite values.
Results may differ from the reference program's by a relative error of at most 0.0083.
Values may be sent and summed in bfloat16 or wider, within the bound.
A program may use at most 64 MiB of HBM per device.

```python
import jax
import jax.numpy as jnp
from jax import lax

D = 2048
H = 16
HEAD = 128
SEQS = 1
POS_DEV = 512
LEN = 8192


def draw_decay_rate(key, part):
    lowest = 1e-05
    highest = 0.06
    uniform_draw = jax.random.uniform(key, (H,), jnp.float32)
    return jnp.exp(jnp.log(lowest) + uniform_draw * (jnp.log(highest) - jnp.log(lowest)))


def shard_levels(rng, extent, pieces, smallest, high):
    def one(position, blocks):
        heights = jax.random.uniform(jax.random.fold_in(jax.random.fold_in(rng, 6), position), (blocks,), jnp.float32, smallest / len(pieces), high / len(pieces))
        return jnp.repeat(jnp.exp(heights), extent[position] // blocks).reshape((-1,) + (1,) * (len(extent) - position - 1))

    level = one(*pieces[0])
    for cut in pieces[1:]:
        level = level * one(*cut)
    return level


def gaussian(rng, shape, scale, reach, shards=(), held_as=jnp.bfloat16):
    result = jax.random.normal(rng, shape, jnp.float32) * scale
    if len(shards) > 0:
        result = shard_levels(rng, shape, shards, -0.22, 0.18) * result
    return jnp.clip(result, min=-reach, max=reach).astype(held_as)


def setup_inputs(seed: int = 0) -> dict:
    seeds = jax.random.split(jax.random.key(seed), 8)
    return {
        "prompt": gaussian(seeds[0], (SEQS, LEN, D), 1.0, 6.0, ((1, 16), (2, 2))),
        "new_token": gaussian(seeds[1], (SEQS, D), 1.0, 6.0, ((1, 2),)),
        "w_query": gaussian(seeds[2], (D, H * HEAD), D ** -0.5, 0.125, ((1, 2),)),
        "w_key": gaussian(seeds[3], (D, H * HEAD), D ** -0.5, 0.125, ((1, 2),)),
        "w_value": gaussian(seeds[4], (D, H * HEAD), D ** -0.5, 0.125, ((1, 2),)),
        "decay_rate": draw_decay_rate(jax.random.fold_in(seeds[7], 71), 0),
        "norm_gain": jnp.clip(1.0 + 0.18 * jax.random.normal(seeds[6], (H * HEAD,), jnp.float32), 0.1, 1.9),
    }


rope_base = 10000.0
norm_floor = 1e-05

def rotate(tensor, positions):
    head_width = tensor.shape[-1]
    inverse = rope_base ** (-jnp.arange(0, head_width, 2, dtype=jnp.float32) / head_width)
    angles = positions.astype(jnp.float32)[:, None] * inverse[None, :]
    cosine = jnp.cos(angles)[:, None, :]
    sine_part = jnp.sin(angles)[:, None, :]
    first_half = tensor[..., :head_width // 2]
    second_half = tensor[..., head_width // 2:]
    return jnp.concatenate([first_half * cosine - second_half * sine_part, first_half * sine_part + second_half * cosine], axis=-1)

def head_norm(output, gain):
    center = lax.optimization_barrier(jnp.mean(output, axis=-1, keepdims=True))
    spread = lax.optimization_barrier(jnp.mean(jnp.square(output - center), axis=-1, keepdims=True))
    return (output - center) * lax.rsqrt(spread + norm_floor) * gain

def decay_tables(log_gamma, block_size):
    offsets = jnp.arange(block_size, dtype=jnp.float32)
    gap_table = offsets[:, None] - offsets[None, :]
    within = jnp.where(gap_table[None] >= 0, jnp.exp(jnp.maximum(gap_table, 0.0)[None] * log_gamma[:, None, None]), 0.0)
    query_decay = jnp.exp((offsets[:, None] + 1.0) * log_gamma[None, :])
    key_decay = jnp.exp((block_size - 1.0 - offsets[:, None]) * log_gamma[None, :])
    return (within, query_decay, key_decay)

def project(token_rows, weight):
    return jnp.dot(token_rows, weight, preferred_element_type=jnp.float32).astype(jnp.bfloat16)

def reference(prompt, new_token, w_query, w_key, w_value, decay_rate, norm_gain):
    sequences, length, model_width = prompt.shape
    block_size = POS_DEV
    blocks = length // block_size
    token_rows = prompt.reshape(sequences * length, model_width)
    full_shape = (sequences, length, H, HEAD)
    queries = project(token_rows, w_query).reshape(full_shape)
    key_rows = project(token_rows, w_key).reshape(full_shape)
    values = project(token_rows, w_value).reshape(full_shape)
    positions = jnp.arange(length, dtype=jnp.int32)
    scaled = (rotate(queries.astype(jnp.float32), positions) * HEAD ** (-0.5)).astype(jnp.bfloat16)
    turned = rotate(key_rows.astype(jnp.float32), positions).astype(jnp.bfloat16)
    log_gamma = -decay_rate
    within, query_decay, key_decay = decay_tables(log_gamma, block_size)
    block_shape = (sequences, blocks, block_size, H, HEAD)

    def to_blocks(tensor):
        return jnp.moveaxis(tensor.reshape(block_shape), 1, 0)
    weighted = (to_blocks(turned).astype(jnp.float32) * key_decay[None, None, :, :, None]).astype(jnp.bfloat16)
    factor = jnp.exp(block_size * log_gamma)

    def advance(state_now, inputs):
        query_block, key_block, weighted_block, value_block = inputs
        scores = jnp.einsum('snhd,smhd->shnm', query_block.astype(jnp.float32), key_block.astype(jnp.float32)) * within[None]
        scores = lax.optimization_barrier(scores.astype(jnp.bfloat16)).astype(jnp.float32)
        inner_part = jnp.einsum('shnm,smhe->snhe', scores, value_block.astype(jnp.float32))
        state_read = lax.optimization_barrier(state_now.astype(jnp.bfloat16)).astype(jnp.float32)
        carried = jnp.einsum('snhd,shde->snhe', query_block.astype(jnp.float32), state_read) * query_decay[None, :, :, None]
        local_state = jnp.einsum('smhd,smhe->shde', weighted_block.astype(jnp.float32), value_block.astype(jnp.float32))
        return (state_now * factor[None, :, None, None] + local_state, inner_part + carried)
    initial = jnp.zeros((sequences, H, HEAD, HEAD), jnp.float32)
    final_state, outputs = lax.scan(advance, initial, (to_blocks(scaled), to_blocks(turned), weighted, to_blocks(values)))
    outputs = jnp.moveaxis(outputs, 0, 1).reshape(full_shape)
    gain = norm_gain.reshape(H, HEAD)
    mixed = head_norm(outputs, gain).astype(jnp.bfloat16).reshape(sequences, length, H * HEAD)
    cache = final_state.astype(jnp.bfloat16)
    token_shape = (sequences, 1, H, HEAD)
    token_query = project(new_token, w_query).reshape(token_shape)
    token_key = project(new_token, w_key).reshape(token_shape)
    token_value = project(new_token, w_value).reshape(token_shape)
    token_positions = jnp.full((1,), length, jnp.int32)
    token_scaled = (rotate(token_query.astype(jnp.float32), token_positions) * HEAD ** (-0.5)).astype(jnp.bfloat16)[:, 0]
    token_turned = rotate(token_key.astype(jnp.float32), token_positions).astype(jnp.bfloat16)[:, 0]
    from_cache = jnp.einsum('shd,shde->she', token_scaled.astype(jnp.float32), final_state, precision=lax.Precision.HIGHEST)
    own_score = lax.optimization_barrier(jnp.sum(token_scaled.astype(jnp.float32) * token_turned.astype(jnp.float32), axis=-1, keepdims=True))
    read_out = jnp.exp(log_gamma)[None, :, None] * from_cache + own_score * token_value[:, 0].astype(jnp.float32)
    new_read = head_norm(read_out, gain).astype(jnp.bfloat16).reshape(sequences, H * HEAD)
    return (mixed, cache, new_read)
```

```python
import functools

import jax
import jax.numpy as jnp
import numpy as np
from jax import lax
from jax.experimental import pallas as pl
from jax.experimental.pallas import tpu as pltpu
from jax.sharding import PartitionSpec as P

HEAD = 128
PAD = 16
rope_base = 10000.0
norm_floor = 1e-05
MESH = pl.DeviceIdType.MESH
BF = jnp.bfloat16
F32 = jnp.float32


def head_norm(o, gain):
    center = jnp.mean(o, axis=-1, keepdims=True)
    delta = o - center
    spread = jnp.mean(delta * delta, axis=-1, keepdims=True)
    return delta * lax.rsqrt(spread + norm_floor) * gain


def split(members):
    best = 1
    for g in range(1, members + 1):
        if members % g == 0 and g * g <= members:
            best = g
    return best


def dot(a, b):
    return jnp.dot(a, b, preferred_element_type=F32)


def kernel(cfg, x_hbm, tok_hbm, wq, wk, wv, rate, gain, tab_hbm, base, mixed, cache, read_out,
           xbuf, tokbuf, wbuf, acc, tab, ctab, stab, kbuf, qbuf, vbuf, intra, obuf,
           send1, recv1, pre, recv2, send3, recv3, pacc, fin, tokq, tokk, tokv, rdbuf,
           w_sem, l_sem, tps, tpr, s1s, s1r, s2s, s2r, s3s, s3r, rds, rdr, o_sem):
    M, G, Z, T, B, F, H, hc, R = cfg
    NC = H // hc
    W = hc * HEAD
    rank = lax.axis_index("sp")
    me = lax.axis_index("tp")
    z = rank // G
    j = rank % G
    weights = (wk, wv, wq)

    lx = pltpu.make_async_copy(x_hbm, xbuf.at[me, pl.ds(0, B)], l_sem.at[0])
    lt = pltpu.make_async_copy(tok_hbm, tokbuf.at[me], l_sem.at[1])
    ltab = pltpu.make_async_copy(tab_hbm, tab, l_sem.at[2])
    lx.start()
    lt.start()

    def wcopy(m, c, d):
        p = lax.rem(me + d, T)
        return pltpu.make_async_copy(
            weights[m].at[pl.ds(pl.multiple_of(p * F, HEAD), F), pl.ds(c * W, W)],
            wbuf.at[m, c, d], w_sem.at[m, c, d])

    for c in range(NC):
        wcopy(0, c, 0).start()
        wcopy(1, c, 0).start()
        if c == 0:
            ltab.start()
    for c in range(NC):
        for d in range(1, T):
            wcopy(0, c, d).start()
            wcopy(1, c, d).start()
    for c in range(NC):
        for d in range(T):
            wcopy(2, c, d).start()

    barrier = pltpu.get_barrier_semaphore()
    for d in range(1, T):
        pl.semaphore_signal(barrier, inc=1, device_id={"tp": lax.rem(me + d, T)}, device_id_type=MESH)
    for d in range(1, M):
        pl.semaphore_signal(barrier, inc=1, device_id={"sp": lax.rem(rank + d, M)}, device_id_type=MESH)

    def widen(p):
        t = tokbuf[p].astype(F32)
        xbuf[p, B:B + PAD, :] = jnp.broadcast_to(t, (PAD, F)).astype(BF)

    lt.wait()
    widen(me)
    lx.wait()

    def own_part(c):
        for m in range(2):
            wcopy(m, c, 0).wait()
            acc[m, c] = dot(xbuf[me], wbuf[m, c, 0])

    own_part(0)
    pl.semaphore_wait(barrier, T - 1 + M - 1)
    sends = []
    for d in range(1, T):
        peer = lax.rem(me + d, T)
        a = pltpu.make_async_remote_copy(
            src_ref=x_hbm, dst_ref=xbuf.at[me, pl.ds(0, B)], send_sem=tps.at[0, d],
            recv_sem=tpr.at[0, d], device_id={"tp": peer}, device_id_type=MESH)
        b = pltpu.make_async_remote_copy(
            src_ref=tok_hbm, dst_ref=tokbuf.at[me], send_sem=tps.at[1, d],
            recv_sem=tpr.at[1, d], device_id={"tp": peer}, device_id_type=MESH)
        a.start()
        b.start()
        sends += [a, b]

    ltab.wait()
    cb = base[rank, 0:1, :]
    sb = base[rank, 1:2, :]
    ctab[0:B, :] = cb * tab[0] - sb * tab[1]
    stab[0:B, :] = sb * tab[0] + cb * tab[1]
    ctab[B:B + PAD, :] = jnp.broadcast_to(base[M, 0:1, :], (PAD, HEAD))
    stab[B:B + PAD, :] = jnp.broadcast_to(base[M, 1:2, :], (PAD, HEAD))

    for c in range(1, NC):
        own_part(c)

    for d in range(1, T):
        src = lax.rem(me + T - d, T)
        pltpu.make_async_remote_copy(
            src_ref=tok_hbm, dst_ref=tokbuf.at[src], send_sem=tps.at[1, d],
            recv_sem=tpr.at[1, d], device_id={"tp": src}, device_id_type=MESH).wait_recv()
        pltpu.make_async_remote_copy(
            src_ref=x_hbm, dst_ref=xbuf.at[src, pl.ds(0, B)], send_sem=tps.at[0, d],
            recv_sem=tpr.at[0, d], device_id={"tp": src}, device_id_type=MESH).wait_recv()
        widen(src)

    def rotated(u):
        return u * ctab[...] + pltpu.roll(u, HEAD // 2, 1) * stab[...]

    def rest(m, c, total):
        for d in range(1, T):
            wcopy(m, c, d).wait()
            part = dot(xbuf[lax.rem(me + d, T)], wbuf[m, c, d])
            total = part if total is None else total + part
        return total

    steps = (lax.broadcasted_iota(jnp.int32, (B, HEAD), 0) + 1).astype(F32)

    def block_decay(c, power):
        rows = [jnp.exp(jnp.full((R, HEAD), -power * B * rate[c * hc + h], F32)) for h in range(hc)]
        return jnp.concatenate(rows, axis=0)

    def phase_kv(c):
        kk = rest(0, c, acc[0, c])
        vv = rest(1, c, acc[1, c])
        states = []
        for hh in range(hc):
            h = c * hc + hh
            cols = slice(hh * HEAD, (hh + 1) * HEAD)
            kr = rotated(kk[:, cols])
            tokk[h:h + 1, :] = kr[B:B + 1]
            krb = kr[:B].astype(BF)
            kbuf[h] = krb
            v = vv[:, cols]
            tokv[h:h + 1, :] = v[B:B + 1]
            vb = (v[:B] * jnp.exp(steps * rate[h])).astype(BF)
            vbuf[h] = vb
            st = lax.dot_general(krb, vb, (((0,), (0,)), ((), ())), preferred_element_type=F32)
            states.append(st * jnp.exp(jnp.full((HEAD, HEAD), -B * rate[h], F32)))
        for i in range(G):
            for zz in range(Z):
                lo = (zz * G + i) * R
                send1[c, i, zz] = jnp.concatenate([s[lo:lo + R] for s in states], axis=0).astype(BF)
        recv1[c, j] = send1[c, j]
        for d in range(1, G):
            i = lax.rem(j + d, G)
            cp = pltpu.make_async_remote_copy(
                src_ref=send1.at[c, i], dst_ref=recv1.at[c, j], send_sem=s1s.at[c, d],
                recv_sem=s1r.at[c, d], device_id={"sp": z * G + i}, device_id_type=MESH)
            cp.start()
            sends.append(cp)

    def full2(c, s, t):
        return pltpu.make_async_remote_copy(
            src_ref=recv2.at[c, s], dst_ref=recv2.at[c, s], send_sem=s2s.at[c, t],
            recv_sem=s2r.at[c, s], device_id={"sp": t * G + j}, device_id_type=MESH)

    def part2(c, s, t):
        return pltpu.make_async_remote_copy(
            src_ref=recv2.at[c, s, t], dst_ref=recv2.at[c, s, t], send_sem=s2s.at[c, t],
            recv_sem=s2r.at[c, s], device_id={"sp": t * G + j}, device_id_type=MESH)

    def phase_plane(c):
        for d in range(1, G):
            i = lax.rem(j + G - d, G)
            pltpu.make_async_remote_copy(
                src_ref=send1.at[c, i], dst_ref=recv1.at[c, i], send_sem=s1s.at[c, d],
                recv_sem=s1r.at[c, d], device_id={"sp": z * G + i}, device_id_type=MESH).wait_recv()
        gb = block_decay(c, 1)[None]
        run = jnp.zeros((Z, hc * R, HEAD), F32)
        for i in range(G):
            pre[c, i] = run
            run = run * gb + recv1[c, i].astype(F32)
        recv2[c, z] = run.astype(BF)
        for t in range(Z):
            @pl.when(t > z)
            def _():
                full2(c, z, t).start()

            @pl.when(t < z)
            def _():
                part2(c, z, t).start()

    def phase_chain(c):
        gz = block_decay(c, G)
        pacc[...] = jnp.zeros((Z, hc * R, HEAD), F32)
        for s in range(Z):
            @pl.when(s < z)
            def _():
                full2(c, s, z).wait_recv()
                pacc[...] = pacc[...] * gz[None] + recv2[c, s].astype(F32)
        run = pacc[...]
        gb = block_decay(c, 1)[None]
        for i in range(G):
            send3[c, i] = (run + pre[c, i]).astype(BF)
            run = run * gb
        recv3[c, j] = send3[c, j]
        for d in range(1, G):
            i = lax.rem(j + d, G)
            cp = pltpu.make_async_remote_copy(
                src_ref=send3.at[c, i], dst_ref=recv3.at[c, j], send_sem=s3s.at[c, d],
                recv_sem=s3r.at[c, d], device_id={"sp": z * G + i}, device_id_type=MESH)
            cp.start()
            sends.append(cp)

    def phase_final(c):
        gz = block_decay(c, G)
        run = jnp.zeros((hc * R, HEAD), F32)
        for s in range(Z):
            @pl.when(s > z)
            def _():
                part2(c, s, z).wait_recv()
            run = run * gz + recv2[c, s, z].astype(F32)
        fin[c * hc * R:(c + 1) * hc * R, :] = run
        for hh in range(hc):
            cache[c * hc + hh] = run[hh * R:(hh + 1) * R].astype(BF)

    half = B // 2
    causal = (lax.broadcasted_iota(jnp.int32, (half, half), 0)
              >= lax.broadcasted_iota(jnp.int32, (half, half), 1))

    def phase_q(c):
        wcopy(2, c, 0).wait()
        qq = rest(2, c, dot(xbuf[me], wbuf[2, c, 0]))
        for hh in range(hc):
            h = c * hc + hh
            qr = rotated(qq[:, hh * HEAD:(hh + 1) * HEAD])
            tokq[h:h + 1, :] = qr[B:B + 1]
            qb = qr[:B].astype(BF)
            qbuf[h] = qb
            for t in range(2):
                rows = qb[t * half:(t + 1) * half]
                out = None
                for s in range(t + 1):
                    ks = kbuf[h, s * half:(s + 1) * half, :]
                    sc = lax.dot_general(rows, ks, (((1,), (1,)), ((), ())), preferred_element_type=F32)
                    if s == t:
                        sc = jnp.where(causal, sc, 0.0)
                    part = dot(sc.astype(BF), vbuf[h, s * half:(s + 1) * half, :])
                    out = part if out is None else out + part
                intra[h, t * half:(t + 1) * half, :] = out

    def phase_tail(c):
        for d in range(1, G):
            i = lax.rem(j + G - d, G)
            pltpu.make_async_remote_copy(
                src_ref=send3.at[c, i], dst_ref=recv3.at[c, i], send_sem=s3s.at[c, d],
                recv_sem=s3r.at[c, d], device_id={"sp": z * G + i}, device_id_type=MESH).wait_recv()
        pieces = [[recv3[c, i, zz].astype(F32) for i in range(G)] for zz in range(Z)]
        for hh in range(hc):
            h = c * hc + hh
            inc = jnp.concatenate(
                [pieces[zz][i][hh * R:(hh + 1) * R] for zz in range(Z) for i in range(G)], axis=0)
            o = intra[h] + dot(qbuf[h], inc.astype(BF))
            o = o * (jnp.exp(steps * -rate[h]) * HEAD ** -0.5)
            res = head_norm(o, gain[:, h * HEAD:(h + 1) * HEAD])
            obuf[c, :, hh * HEAD:(hh + 1) * HEAD] = res.astype(BF)
        pltpu.make_async_copy(obuf.at[c], mixed.at[:, pl.ds(c * W, W)], o_sem.at[c]).start()

    def read_send():
        tq = tokq[...].astype(BF).astype(F32)
        n = H * R
        pick = (lax.broadcasted_iota(jnp.int32, (HEAD, n), 0)
                == rank * R + lax.broadcasted_iota(jnp.int32, (HEAD, n), 1) % R)
        sel = dot(tq, pick.astype(F32))
        own = (lax.broadcasted_iota(jnp.int32, (H, n), 0)
               == lax.broadcasted_iota(jnp.int32, (H, n), 1) // R)
        sel = jnp.where(own, sel, 0.0)
        rdbuf[rank] = jnp.dot(sel, fin[...], preferred_element_type=F32, precision=lax.Precision.HIGHEST)
        for d in range(1, M):
            peer = lax.rem(rank + d, M)
            cp = pltpu.make_async_remote_copy(
                src_ref=rdbuf.at[rank], dst_ref=rdbuf.at[rank], send_sem=rds.at[d],
                recv_sem=rdr.at[d], device_id={"sp": peer}, device_id_type=MESH)
            cp.start()
            sends.append(cp)

    def read_finish():
        for d in range(1, M):
            src = lax.rem(rank + M - d, M)
            pltpu.make_async_remote_copy(
                src_ref=rdbuf.at[src], dst_ref=rdbuf.at[src], send_sem=rds.at[d],
                recv_sem=rdr.at[d], device_id={"sp": src}, device_id_type=MESH).wait_recv()
        total = jnp.sum(rdbuf[...], axis=0)
        scale = HEAD ** -0.5
        tq = tokq[...].astype(BF).astype(F32)
        tk = tokk[...].astype(BF).astype(F32)
        score = jnp.sum(tq * tk, axis=-1, keepdims=True) * scale
        base_part = score * tokv[...].astype(BF).astype(F32)
        for h in range(H):
            g = jnp.exp(jnp.full((1, HEAD), -rate[h], F32)) * scale
            o = g * total[h:h + 1] + base_part[h:h + 1]
            read_out[:, h * HEAD:(h + 1) * HEAD] = head_norm(o, gain[:, h * HEAD:(h + 1) * HEAD]).astype(BF)

    work = [functools.partial(phase_kv, c) for c in range(NC)]
    work += [functools.partial(phase_q, c) for c in range(NC)]
    plane_at, chain_at = 2, 5
    planes = 0
    chains = 0
    for n, step in enumerate(work):
        step()
        if n >= plane_at and planes < NC and planes <= n:
            phase_plane(planes)
            planes += 1
        if n >= chain_at and chains < planes:
            phase_chain(chains)
            chains += 1
    while planes < NC:
        phase_plane(planes)
        planes += 1
    while chains < NC:
        phase_chain(chains)
        chains += 1
    for c in range(NC):
        phase_final(c)
    read_send()
    for c in range(NC):
        phase_tail(c)
    read_finish()
    for cp in sends:
        cp.wait_send()
    for c in range(NC):
        for t in range(Z):
            @pl.when(t > z)
            def _():
                full2(c, z, t).wait_send()

            @pl.when(t < z)
            def _():
                part2(c, z, t).wait_send()
        pltpu.make_async_copy(obuf.at[c], mixed.at[:, pl.ds(c * W, W)], o_sem.at[c]).wait()


def per_device(prompt, new_token, w_query, w_key, w_value, decay_rate, norm_gain):
    _, B, F = prompt.shape
    D = w_query.shape[0]
    H = w_query.shape[1] // HEAD
    M = lax.axis_size("sp")
    T = lax.axis_size("tp")
    G = split(M)
    Z = M // G
    R = HEAD // M
    hc = 2 if H % 2 == 0 else 1
    NC = H // hc
    W = hc * HEAD
    inverse = rope_base ** (-np.arange(0, HEAD, 2, dtype=np.float64) / HEAD)
    sign = np.concatenate([-np.ones(HEAD // 2), np.ones(HEAD // 2)])

    def pair(positions):
        angles = np.concatenate([positions[:, None] * inverse[None]] * 2, axis=1)
        return np.cos(angles), np.sin(angles) * sign[None]

    tab = np.stack(pair(np.arange(B, dtype=np.float64))).astype(np.float32)
    base = np.stack(pair(np.arange(M + 1, dtype=np.float64) * B), axis=1).astype(np.float32)
    any_ = pl.BlockSpec(memory_space=pltpu.HBM)
    vm = pl.BlockSpec(memory_space=pltpu.VMEM)
    sm = pl.BlockSpec(memory_space=pltpu.SMEM)
    V = pltpu.VMEM
    DMA = pltpu.SemaphoreType.DMA
    cfg = (M, G, Z, T, B, F, H, hc, R)
    mixed, cache, new_read = pl.pallas_call(
        functools.partial(kernel, cfg),
        out_shape=(
            jax.ShapeDtypeStruct((B, H * HEAD), BF),
            jax.ShapeDtypeStruct((H, R, HEAD), BF),
            jax.ShapeDtypeStruct((1, H * HEAD), BF),
        ),
        in_specs=[any_, any_, any_, any_, any_, sm, vm, any_, vm],
        out_specs=(any_, vm, vm),
        scratch_shapes=[
            V((T, B + PAD, F), BF),
            V((T, 1, F), BF),
            V((3, NC, T, F, W), BF),
            V((2, NC, B + PAD, W), F32),
            V((2, B, HEAD), F32),
            V((B + PAD, HEAD), F32),
            V((B + PAD, HEAD), F32),
            V((H, B, HEAD), BF),
            V((H, B, HEAD), BF),
            V((H, B, HEAD), BF),
            V((H, B, HEAD), F32),
            V((NC, B, W), BF),
            V((NC, G, Z, hc * R, HEAD), BF),
            V((NC, G, Z, hc * R, HEAD), BF),
            V((NC, G, Z, hc * R, HEAD), F32),
            V((NC, Z, Z, hc * R, HEAD), BF),
            V((NC, G, Z, hc * R, HEAD), BF),
            V((NC, G, Z, hc * R, HEAD), BF),
            V((Z, hc * R, HEAD), F32),
            V((H * R, HEAD), F32),
            V((H, HEAD), F32),
            V((H, HEAD), F32),
            V((H, HEAD), F32),
            V((M, H, HEAD), F32),
            DMA((3, NC, T)),
            DMA((3,)),
            DMA((2, T)),
            DMA((2, T)),
            DMA((NC, G)),
            DMA((NC, G)),
            DMA((NC, Z)),
            DMA((NC, Z)),
            DMA((NC, G)),
            DMA((NC, G)),
            DMA((M,)),
            DMA((M,)),
            DMA((NC,)),
        ],
        compiler_params=pltpu.CompilerParams(
            collective_id=0, has_side_effects=True, vmem_limit_bytes=60 * 1024 * 1024),
    )(prompt.reshape(B, F), new_token, w_query, w_key, w_value, decay_rate,
      norm_gain.reshape(1, H * HEAD), jnp.asarray(tab), jnp.asarray(base))
    return (mixed[None], cache[None], new_read)


def solution(mesh):
    in_specs = (
        P(None, "sp", "tp"),
        P(None, "tp"),
        P(None, "tp"),
        P(None, "tp"),
        P(None, "tp"),
        P("tp"),
        P("tp"),
    )
    out_specs = (P(None, "sp", "tp"), P(None, "tp", "sp", None), P(None, "tp"))
    return jax.shard_map(
        per_device, mesh=mesh, in_specs=in_specs, out_specs=out_specs, check_vma=False
    )
```
